32 devices in a mesh: sp: 8 (over z, x), tp: 4 (over y, core).
Axes of the slice: x: 2, y: 2, z: 4, core: 2. Of those that a mesh axis runs over, the one named last changes fastest.
Arguments:
- tokens: bfloat16 [1024, 2048], P('sp', 'tp'), may hold values from -6 to 6
- input_norm_gain: float32 [2048], replicated, may hold values from 0.1 to 1.9
- delta_query_projection: bfloat16 [2048, 512], P('sp', 'tp'), may hold values from -0.125 to 0.125
- delta_key_projection: bfloat16 [2048, 512], P('sp', 'tp'), may hold values from -0.125 to 0.125
- delta_value_projection: bfloat16 [2048, 512], P('sp', 'tp'), may hold values from -0.125 to 0.125
- delta_gate_projection: bfloat16 [2048, 512], P('sp', 'tp'), may hold values from -0.125 to 0.125
- write_strength_weight: bfloat16 [2048, 8], replicated, may hold values from -0.125 to 0.125
- decay_projection: bfloat16 [2048, 8], replicated, may hold values from -0.125 to 0.125
- write_strength_bias: float32 [8], P('tp'), as said below
- decay_scale_per_head: float32 [8], P('tp'), may hold values from 0 to 1
- decay_offset_terms: float32 [1024, 8], P('sp', 'tp'), may hold values from -1 to 0
- delta_norm_gain: float32 [64], replicated, may hold values from 0.1 to 1.9
- delta_output_projection: bfloat16 [2048, 512], P('sp', 'tp'), may hold values from -0.25 to 0.25
- window_query_projection: bfloat16 [2048, 1024], P('sp', 'tp'), may hold values from -1 to 1
- window_key_projection: bfloat16 [2048, 256], P('sp', 'tp'), may hold values from -1 to 1
- window_value_projection: bfloat16 [2048, 256], P('sp', 'tp'), may hold values from -0.125 to 0.125
- window_sink_logits: float32 [16], P('tp'), may hold values from 1 to 6
- window_output_projection: bfloat16 [2048, 1024], P('sp', 'tp'), may hold values from -0.1875 to 0.1875
Outputs:
- mixed: bfloat16 [1024, 2048], P(('sp', 'tp'))
- log_totals: float32 [1024, 16], P('sp', 'tp')
The draws below stay inside these ranges and needn't reach their ends.
Inputs may be any that keep to these rules, and one draw needn't show every extreme that they name: `write_strength_bias`: at least the logarithm of 4 / 1024.
All inputs are finite; a program needn't handle non-finite values.
Results may differ from the reference program's by a relative error of at most 0.023.
The reference program's roundings to bfloat16 on the way count: a program that leaves them out, or rounds other values in their place, can miss the bound.
Values may be sent and summed in bfloat16 or wider, within the bound.
A program may use at most 64 MiB of HBM per device.

```python
import jax
import jax.numpy as jnp
from jax import lax

D = 2048
E = 64
HG = 8
HQ = 16
HK = 4
WINDOW = 128
DELTA_BLOCK_SIZE = 64
TOK_DEV = 128
TOKENS = 1024
N_TP = 4


def slow_marks(key):
    ranks = jax.random.permutation(jax.random.fold_in(key, 3), HG)
    return ranks < HG // 2


def draw_decay_scale_per_head(key, part):
    slow = slow_marks(key)
    level = jax.random.uniform(jax.random.fold_in(key, 5), (HG,), jnp.float32)
    return jnp.where(slow, (0.1 + 0.1 * level) / TOKENS, 0.02 + 0.04 * level)


def draw_write_strength_bias(key, part):
    slow = slow_marks(key)
    level = jax.random.uniform(jax.random.fold_in(key, 6), (HG,), jnp.float32)
    return jnp.where(slow, jnp.log((4.0 + 4.0 * level) / TOKENS), 2.0 * level - 1.0)


def draw_decay_offset_terms(key, part):
    device_blocks = TOKENS // TOK_DEV
    spread = jax.random.uniform(jax.random.fold_in(key, 8), (device_blocks, HG), jnp.float32, -1.3862944, 0.0)
    baseline_result = -jnp.repeat(jnp.exp(spread), TOK_DEV, axis=0) / TOKENS
    position_indices = jax.random.randint(jax.random.fold_in(key, 9), (2, HG), 0, TOKENS)
    layer_depth = jnp.log(jax.random.uniform(jax.random.fold_in(key, 10), (2, HG), jnp.float32, 0.5, 0.8))
    row_position_index = jnp.arange(TOKENS, dtype=jnp.int32)[:, None]
    first_offset_draw = jnp.where(row_position_index == position_indices[0][None, :], layer_depth[0][None, :], 0.0)
    second_offset_draw = jnp.where(row_position_index == position_indices[1][None, :], layer_depth[1][None, :], 0.0)
    return baseline_result + first_offset_draw + second_offset_draw


def loud_scale(key, columns_each):
    per_head = jnp.ones((HK,), jnp.float32)
    return jnp.repeat(per_head, columns_each)


def draw_window_query_projection(key, part):
    scaling = loud_scale(key, HQ // HK * E)
    entries = jax.random.normal(jax.random.fold_in(key, 11), (D, HQ * E), jnp.float32) * D ** (-0.5) * scaling[None, :]
    return jnp.clip(entries, -1.0, 1.0).astype(jnp.bfloat16)


def draw_window_key_projection(key, part):
    scaling = loud_scale(key, E)
    entries = jax.random.normal(jax.random.fold_in(key, 13), (D, HK * E), jnp.float32) * D ** (-0.5) * scaling[None, :]
    return jnp.clip(entries, -1.0, 1.0).astype(jnp.bfloat16)


def block_scale(key, dims, split, least, top_value):
    level = 1.0
    for dim, blocks in split:
        steps = jax.random.uniform(jax.random.fold_in(jax.random.fold_in(key, 6), dim), (blocks,), jnp.float32, least / len(split), top_value / len(split))
        level = level * jnp.repeat(jnp.exp(steps), dims[dim] // blocks).reshape((-1,) + (1,) * (len(dims) - 1 - dim))
    return level


def bell_draw(rng, extent, scale, most, pieces=(), held_as=jnp.bfloat16):
    gain = block_scale(rng, extent, pieces, -0.22, 0.18) if pieces else 1.0
    array = jax.random.normal(rng, extent, jnp.float32) * scale * gain
    return jnp.minimum(jnp.maximum(array, -most), most).astype(held_as)


def setup_inputs(seed: int = 0) -> dict:
    key_list = jax.random.split(jax.random.key(seed), 19)
    tokens = bell_draw(key_list[0], (TOKENS, D), 1.0, 6.0, ((0, 8), (1, 4)))
    input_norm_gain = jnp.clip(1.0 + 0.18 * jax.random.normal(key_list[1], (D,), jnp.float32), 0.1, 1.9)
    delta_query_projection = bell_draw(key_list[2], (D, HG * E), D ** -0.5, 0.125, ((0, 8), (1, 4)))
    delta_key_projection = bell_draw(key_list[3], (D, HG * E), D ** -0.5, 0.125, ((0, 8), (1, 4)))
    delta_value_projection = bell_draw(key_list[4], (D, HG * E), D ** -0.5, 0.125, ((0, 8), (1, 4)))
    delta_gate_projection = bell_draw(key_list[5], (D, HG * E), D ** -0.5, 0.125, ((0, 8), (1, 4)))
    write_strength_weight = bell_draw(key_list[6], (D, HG), D ** -0.5, 0.125)
    decay_projection = bell_draw(key_list[7], (D, HG), D ** -0.5, 0.125)
    write_strength_bias = draw_write_strength_bias(jax.random.fold_in(key_list[18], 71), 0)
    decay_scale_per_head = draw_decay_scale_per_head(jax.random.fold_in(key_list[18], 71), 0)
    decay_offset_terms = draw_decay_offset_terms(jax.random.fold_in(key_list[18], 71), 0)
    delta_norm_gain = jnp.clip(1.0 + 0.18 * jax.random.normal(key_list[11], (E,), jnp.float32), 0.1, 1.9)
    delta_output_projection = bell_draw(key_list[12], (D, HG * E), (HG * E) ** -0.5, 0.25, ((0, 8), (1, 4)))
    window_query_projection = draw_window_query_projection(jax.random.fold_in(key_list[18], 71), 0)
    window_key_projection = draw_window_key_projection(jax.random.fold_in(key_list[18], 71), 0)
    window_value_projection = bell_draw(key_list[15], (D, HK * E), D ** -0.5, 0.125, ((0, 8), (1, 4)))
    window_sink_logits = jnp.clip(1.0 + 5.0 * jax.random.uniform(key_list[16], (HQ,), jnp.float32) ** block_scale(key_list[16], (HQ,), ((0, 4),), -0.2, 0.2), 1.0, 6.0)
    window_output_projection = bell_draw(key_list[17], (D, HQ * E), (HQ * E) ** -0.5, 0.1875, ((0, 8), (1, 4)))
    return dict(tokens=tokens, input_norm_gain=input_norm_gain, delta_query_projection=delta_query_projection, delta_key_projection=delta_key_projection, delta_value_projection=delta_value_projection, delta_gate_projection=delta_gate_projection, write_strength_weight=write_strength_weight, decay_projection=decay_projection, write_strength_bias=write_strength_bias, decay_scale_per_head=decay_scale_per_head, decay_offset_terms=decay_offset_terms, delta_norm_gain=delta_norm_gain, delta_output_projection=delta_output_projection, window_query_projection=window_query_projection, window_key_projection=window_key_projection, window_value_projection=window_value_projection, window_sink_logits=window_sink_logits, window_output_projection=window_output_projection)


epsilon = 1e-06
rope_base = 500000.0
highest = lax.Precision.HIGHEST

def unit_rows(values):
    return values * lax.rsqrt(lax.optimization_barrier(jnp.sum(values * values, axis=-1, keepdims=True)) + epsilon)

def rotate(values, positions):
    head_size = values.shape[-1]
    half_size = head_size // 2
    frequency = rope_base ** (-(2.0 / head_size) * jnp.arange(half_size, dtype=jnp.float32))
    angles = positions.astype(jnp.float32)[:, None] * frequency[None, :]
    cosine = jnp.cos(angles)[:, None, :]
    sine_part = jnp.sin(angles)[:, None, :]
    first_half = values[..., :half_size]
    second_half = values[..., half_size:]
    return jnp.concatenate([first_half * cosine - second_half * sine_part, second_half * cosine + first_half * sine_part], axis=-1)

def delta_rule_mixer(query_accumulator, key_accumulator, value_accumulator, gate_accumulator, rate_preactivation, write_strength_bias, decay_scale_per_head, decay_offset_terms, delta_norm_gain):
    total_rows = query_accumulator.shape[0]
    number_of_heads = write_strength_bias.shape[0]
    block_list = total_rows // DELTA_BLOCK_SIZE

    def heads_first(values):
        return values.reshape(block_list, DELTA_BLOCK_SIZE, number_of_heads, E).transpose(2, 0, 1, 3)
    queries = unit_rows(heads_first(jax.nn.silu(query_accumulator))) * E ** (-0.5)
    key_rows = unit_rows(heads_first(jax.nn.silu(key_accumulator)))
    values = heads_first(jax.nn.silu(value_accumulator))
    write_rate = jax.nn.sigmoid(rate_preactivation[:, :number_of_heads] + write_strength_bias).T.reshape(number_of_heads, block_list, DELTA_BLOCK_SIZE)
    decay_logarithm = (decay_offset_terms - decay_scale_per_head * jax.nn.softplus(rate_preactivation[:, number_of_heads:])).T.reshape(number_of_heads, block_list, DELTA_BLOCK_SIZE)
    cumulative = jnp.cumsum(decay_logarithm, axis=-1)
    offsets_in = jnp.arange(DELTA_BLOCK_SIZE)
    lower_mask = offsets_in[:, None] >= offsets_in[None, :]
    strict = offsets_in[:, None] > offsets_in[None, :]
    within = jnp.where(lower_mask, cumulative[..., :, None] - cumulative[..., None, :], 0.0)
    decay_matrix = jnp.where(lower_mask, jnp.exp(within), 0.0)
    keys_written = key_rows * write_rate[..., None]
    key_gram = jnp.einsum('hncd,hnsd->hncs', keys_written, key_rows, precision=highest) * decay_matrix
    system = jnp.eye(DELTA_BLOCK_SIZE, dtype=jnp.float32) + jnp.where(strict, key_gram, 0.0)
    right_side = jnp.concatenate([values * write_rate[..., None], keys_written * jnp.exp(cumulative)[..., None]], axis=-1)
    solved = jax.scipy.linalg.solve_triangular(system, right_side, lower=True)
    update_values = solved[..., :E]
    update_keys = solved[..., E:]
    scores = jnp.einsum('hncd,hnsd->hncs', queries, key_rows, precision=highest) * decay_matrix
    queries_decayed = queries * jnp.exp(cumulative)[..., None]
    last_gate = cumulative[..., -1]
    keys_decayed = key_rows * jnp.exp(last_gate[..., None] - cumulative)[..., None]

    def advance(memory, inputs):
        value_block, weight_block, score_block, query_block, key_block, gate_block = inputs
        corrected = value_block - jnp.einsum('hcd,hde->hce', weight_block, memory, precision=highest)
        output = jnp.einsum('hcd,hde->hce', query_block, memory, precision=highest) + jnp.einsum('hcs,hse->hce', score_block, corrected, precision=highest)
        memory = memory * jnp.exp(gate_block)[:, None, None] + jnp.einsum('hcd,hce->hde', key_block, corrected, precision=highest)
        return (memory, output)
    inputs = tuple((jnp.moveaxis(tensor, 1, 0) for tensor in (update_values, update_keys, scores, queries_decayed, keys_decayed, last_gate)))
    unused, outputs = lax.scan(advance, jnp.zeros((number_of_heads, E, E), jnp.float32), inputs)
    outputs = outputs.transpose(0, 2, 1, 3).reshape(total_rows, number_of_heads, E)
    normalized = outputs * lax.rsqrt(lax.optimization_barrier(jnp.mean(outputs * outputs, axis=-1, keepdims=True)) + epsilon) * delta_norm_gain
    gated = normalized * jax.nn.silu(gate_accumulator).reshape(total_rows, number_of_heads, E)
    return gated.astype(jnp.bfloat16).reshape(total_rows, number_of_heads * E)

def window_mixer(query_accumulator, key_accumulator, value_accumulator, window_sink_logits):
    total_rows = query_accumulator.shape[0]
    group_size = HQ // HK
    block_list = total_rows // WINDOW
    positions = jnp.arange(total_rows, dtype=jnp.int32)
    queries = rotate(query_accumulator.reshape(total_rows, HQ, E), positions).astype(jnp.bfloat16)
    key_rows = rotate(key_accumulator.reshape(total_rows, HK, E), positions).astype(jnp.bfloat16)
    value_rows = value_accumulator.reshape(total_rows, HK, E).astype(jnp.bfloat16)
    padding = jnp.zeros((WINDOW, HK, E), jnp.bfloat16)

    def banded(rows_in):
        extended = jnp.concatenate([padding, rows_in], axis=0).reshape(block_list + 1, WINDOW, HK, E)
        return jnp.concatenate([extended[:-1], extended[1:]], axis=1).transpose(2, 0, 1, 3)
    query_blocks = queries.reshape(block_list, WINDOW, HK, group_size, E).transpose(2, 0, 1, 3, 4)
    query_in = jnp.arange(WINDOW)[:, None]
    key_in = jnp.arange(2 * WINDOW)[None, :]
    key_start = (jnp.arange(block_list) - 1) * WINDOW
    visible = ((key_in <= query_in + WINDOW) & (key_in > query_in))[None] & (key_start[:, None, None] + key_in[None] >= 0)
    visible = visible[:, None]

    def one_head(inputs):
        query_head, key_head, value_head, sink_head = inputs
        scores = jnp.einsum('nqgd,nkd->ngqk', query_head.astype(jnp.float32), key_head.astype(jnp.float32)) * E ** (-0.5)
        sink_rows = sink_head[None, :, None]
        row_top = jnp.maximum(lax.optimization_barrier(jnp.max(jnp.where(visible, scores, -jnp.inf), axis=-1)), sink_rows)
        weights = jnp.where(visible, jnp.exp(scores - row_top[..., None]), 0.0)
        row_total = lax.optimization_barrier(jnp.sum(weights, axis=-1)) + jnp.exp(sink_rows - row_top)
        weights_low = (weights / row_total[..., None]).astype(jnp.bfloat16)
        mixed_rows = jnp.einsum('ngqk,nkd->nqgd', weights_low.astype(jnp.float32), value_head.astype(jnp.float32)).astype(jnp.bfloat16)
        return (mixed_rows, row_top + jnp.log(row_total))
    mixed_rows, log_totals = lax.map(one_head, (query_blocks, banded(key_rows), banded(value_rows), window_sink_logits.reshape(HK, group_size)))
    mixed_rows = mixed_rows.transpose(1, 2, 0, 3, 4).reshape(total_rows, HQ * E)
    log_totals = log_totals.transpose(1, 3, 0, 2).reshape(total_rows, HQ)
    return (mixed_rows, log_totals)

def reference(tokens, input_norm_gain, delta_query_projection, delta_key_projection, delta_value_projection, delta_gate_projection, write_strength_weight, decay_projection, write_strength_bias, decay_scale_per_head, decay_offset_terms, delta_norm_gain, delta_output_projection, window_query_projection, window_key_projection, window_value_projection, window_sink_logits, window_output_projection):
    widened = tokens.astype(jnp.float32)
    normed = (widened * lax.rsqrt(lax.optimization_barrier(jnp.mean(widened * widened, axis=1, keepdims=True)) + epsilon) * input_norm_gain).astype(jnp.bfloat16)

    def apply_projection(weight):
        return jnp.dot(normed.astype(jnp.float32), weight.astype(jnp.float32), preferred_element_type=jnp.float32)
    rate_preactivation = jnp.concatenate([apply_projection(write_strength_weight), apply_projection(decay_projection)], axis=1)
    delta_mixed_output = delta_rule_mixer(apply_projection(delta_query_projection), apply_projection(delta_key_projection), apply_projection(delta_value_projection), apply_projection(delta_gate_projection), rate_preactivation, write_strength_bias, decay_scale_per_head, decay_offset_terms, delta_norm_gain)
    window_mix, log_totals = window_mixer(apply_projection(window_query_projection), apply_projection(window_key_projection), apply_projection(window_value_projection), window_sink_logits)
    delta_cols = HG * E // N_TP
    window_cols = HQ * E // N_TP
    mixed = jnp.zeros((TOKENS, D), jnp.float32)
    for group_index in range(N_TP):
        delta_part = delta_mixed_output[:, group_index * delta_cols:(group_index + 1) * delta_cols]
        delta_weight = delta_output_projection[:, group_index * delta_cols:(group_index + 1) * delta_cols]
        window_part = window_mix[:, group_index * window_cols:(group_index + 1) * window_cols]
        window_weight = window_output_projection[:, group_index * window_cols:(group_index + 1) * window_cols]
        partial_sum = jnp.dot(delta_part.astype(jnp.float32), delta_weight.T.astype(jnp.float32), preferred_element_type=jnp.float32) + jnp.dot(window_part.astype(jnp.float32), window_weight.T.astype(jnp.float32), preferred_element_type=jnp.float32)
        rounded = lax.optimization_barrier(partial_sum.astype(jnp.bfloat16))
        mixed = mixed + rounded.astype(jnp.float32)
    return (mixed.astype(jnp.bfloat16), log_totals)
```

```python
import functools

import jax
import jax.numpy as jnp
from jax import lax
from jax.experimental import pallas as pl
from jax.experimental.pallas import tpu as pltpu
from jax.sharding import PartitionSpec as P

WINDOW = 128
epsilon = 1e-06
rope_base = 500000.0
highest = lax.Precision.HIGHEST
MESH = pl.DeviceIdType.MESH
f32 = jnp.float32
bf16 = jnp.bfloat16


def dot_nn(a, b, precision=highest):
    return lax.dot_general(a, b, (((1,), (0,)), ((), ())), precision=precision, preferred_element_type=f32)


def dot_nt(a, b, precision=highest):
    return lax.dot_general(a, b, (((1,), (1,)), ((), ())), precision=precision, preferred_element_type=f32)


def dot_tn(a, b, precision=highest):
    return lax.dot_general(a, b, (((0,), (0,)), ((), ())), precision=precision, preferred_element_type=f32)


def silu(u):
    return u / (1.0 + jnp.exp(-u))


def unit_rows(u):
    return u * lax.rsqrt(jnp.sum(u * u, axis=-1, keepdims=True) + epsilon)


def iota(shape, dim):
    return lax.broadcasted_iota(jnp.int32, shape, dim)


def layer_kernel(
    S, T, G,
    tok_ref, gain_ref, dq_ref, dk_ref, dv_ref, dz_ref, ww_ref, wd_ref, bias_ref, scale_ref, offs_ref,
    ngain_ref, do_ref, wq_ref, wk_ref, wv_ref, sink_ref, wo_ref,
    mixed_ref, logt_ref,
    tokbuf, normed, Wd, Ww, Wo, st, edge_own, edge_in, mix, part, partin, memory,
    local_sem, tok_send, tok_recv, w_send, w_recv, st_send, st_recv, edge_send, edge_recv, out_send, out_recv,
):
    me = lax.axis_index("sp")
    j = lax.axis_index("tp")
    Z = S // G
    z = me // G
    x = me % G
    R, F = tok_ref.shape
    rows = dq_ref.shape[0]
    dc = dq_ref.shape[1]
    qc = wq_ref.shape[1]
    kc = wk_ref.shape[1]
    H = bias_ref.shape[0]
    E = dc // H
    QH = sink_ref.shape[0]
    mine = pl.ds(pl.multiple_of(me * rows, rows), rows)

    def local(i, src, dst):
        return pltpu.make_async_copy(src, dst, local_sem.at[i])

    locals_ = [
        local(0, dq_ref, Wd.at[mine, pl.ds(0, dc)]),
        local(1, dk_ref, Wd.at[mine, pl.ds(dc, dc)]),
        local(2, dv_ref, Wd.at[mine, pl.ds(2 * dc, dc)]),
        local(3, dz_ref, Wd.at[mine, pl.ds(3 * dc, dc)]),
        local(4, wq_ref, Ww.at[mine, pl.ds(0, qc)]),
        local(5, do_ref, Wo.at[mine, pl.ds(0, dc)]),
        local(6, wo_ref, Wo.at[mine, pl.ds(dc, qc)]),
        local(7, tok_ref, tokbuf.at[j]),
    ]
    for c in locals_:
        c.start()
    Ww[mine, pl.ds(qc, 2 * kc)] = jnp.concatenate([wk_ref[...], wv_ref[...]], axis=1)

    barrier = pltpu.get_barrier_semaphore()

    def greet_sp(d, _):
        pl.semaphore_signal(barrier, inc=1, device_id={"sp": lax.rem(me + d, S)}, device_id_type=MESH)
        return 0

    lax.fori_loop(1, S, greet_sp, 0)
    for d in range(1, T):
        pl.semaphore_signal(barrier, inc=1, device_id={"tp": lax.rem(j + d, T)}, device_id_type=MESH)
    pl.semaphore_wait(barrier, S - 1 + T - 1)

    def tok_copy(d):
        return pltpu.make_async_remote_copy(
            src_ref=tok_ref, dst_ref=tokbuf.at[j], send_sem=tok_send.at[d], recv_sem=tok_recv.at[j],
            device_id={"tp": lax.rem(j + d, T)}, device_id_type=MESH)

    for d in range(1, T):
        tok_copy(d).start()

    bufs = (Wd, Ww, Wo)

    def slab(g, p):
        return bufs[g].at[pl.ds(pl.multiple_of(p * rows, rows), rows), :]

    def wcopy(g, p, way):
        target = (me + G, me - G, me - x + lax.rem(x + 1, G))[way]
        return pltpu.make_async_remote_copy(
            src_ref=slab(g, p), dst_ref=slab(g, p), send_sem=w_send.at[g, way, p // G], recv_sem=w_recv.at[g, p],
            device_id={"sp": target}, device_id_type=MESH)

    def wait_slab(g, p):
        wcopy(g, p, 2 if G > 1 else 0).wait_recv()

    def forward(g, p, up, down):
        if up:
            @pl.when(z + 1 < Z)
            def _():
                wcopy(g, p, 0).start()
        if down:
            @pl.when(z > 0)
            def _():
                wcopy(g, p, 1).start()
        if G > 1:
            wcopy(g, p, 2).start()

    def relay(g, t):
        @pl.when(z - t >= 0)
        def _():
            p = (z - t) * G + x
            wait_slab(g, p)
            forward(g, p, True, False)

        @pl.when(z + t < Z)
        def _():
            p = (z + t) * G + x
            wait_slab(g, p)
            forward(g, p, False, True)

    def relays(g, low, high):
        def one(t, _):
            relay(g, t)
            return 0
        lax.fori_loop(low, high, one, 0)

    def finish(g):
        if G > 1:
            def one(zz, _):
                wait_slab(g, zz * G + lax.rem(x + 1, G))
                return 0
            lax.fori_loop(0, Z, one, 0)

    def drain(g):
        def one(zz, _):
            p = zz * G + x

            @pl.when((zz <= z) & (z + 1 < Z))
            def _():
                wcopy(g, p, 0).wait_send()

            @pl.when((zz >= z) & (z > 0))
            def _():
                wcopy(g, p, 1).wait_send()

            if G > 1:
                wcopy(g, p, 2).wait_send()
            return 0
        lax.fori_loop(0, Z, one, 0)

    for i in range(4):
        locals_[i].wait()
    forward(0, me, True, True)
    locals_[4].wait()
    forward(1, me, True, True)
    for i in (5, 6):
        locals_[i].wait()
    forward(2, me, True, True)

    half = E // 2
    lane = iota((R, E), 1)
    pair = jnp.where(lane < half, lane, lane - half).astype(f32)
    frequency = jnp.exp(pair * (-(2.0 / E)) * jnp.log(jnp.full((R, E), rope_base, f32)))
    angle = (me * R + iota((R, E), 0)).astype(f32) * frequency
    cosine = jnp.cos(angle)
    sine = jnp.sin(angle)
    ei = iota((E, E), 0)
    ej = iota((E, E), 1)
    swap = jnp.where(ei == ej + half, -1.0, 0.0) + jnp.where(ej == ei + half, 1.0, 0.0)

    locals_[7].wait()
    for d in range(1, T):
        src = lax.rem(j + d, T)
        pltpu.make_async_remote_copy(
            src_ref=tok_ref, dst_ref=tokbuf.at[src], send_sem=tok_send.at[d], recv_sem=tok_recv.at[src],
            device_id={"tp": lax.rem(j + d, T)}, device_id_type=MESH).wait_recv()
    total = jnp.zeros((R, 1), f32)
    for t in range(T):
        u = tokbuf[t].astype(f32)
        total = total + jnp.sum(u * u, axis=1, keepdims=True)
    inverse = lax.rsqrt(total / (T * F) + epsilon)
    for t in range(T):
        normed[:, t * F:(t + 1) * F] = (
            tokbuf[t].astype(f32) * inverse * gain_ref[:, t * F:(t + 1) * F]).astype(bf16)
    pre_w = jnp.dot(normed[...], ww_ref[...], preferred_element_type=f32)
    pre_d = jnp.dot(normed[...], wd_ref[...], preferred_element_type=f32)
    all_heads = pre_w.shape[1]
    head_lane = iota((R, all_heads), 1)

    relays(0, 1, Z)
    finish(0)
    proj = jnp.dot(normed[...], Wd[...], preferred_element_type=f32)

    ri = iota((R, R), 0)
    rj = iota((R, R), 1)
    lower = ri >= rj
    strict = ri > rj
    tril = jnp.where(lower, 1.0, 0.0)
    levels = []
    size = 1
    while size < R:
        levels.append(strict & (ri // (2 * size) == rj // (2 * size)) & (ri // size != rj // size))
        size *= 2
    keep = []
    for h in range(H):
        def head(n):
            return proj[:, n * dc + h * E:n * dc + (h + 1) * E]
        q = unit_rows(silu(head(0))) * E ** (-0.5)
        k = unit_rows(silu(head(1)))
        v = silu(head(2))
        chosen = head_lane == j * H + h
        write = jnp.sum(jnp.where(chosen, pre_w, 0.0), axis=1, keepdims=True) + bias_ref[h]
        decay = jnp.sum(jnp.where(chosen, pre_d, 0.0), axis=1, keepdims=True)
        beta = 1.0 / (1.0 + jnp.exp(-write))
        soft = jnp.maximum(decay, 0.0) + jnp.log1p(jnp.exp(-jnp.abs(decay)))
        logd = offs_ref[:, h:h + 1] - scale_ref[h] * soft
        C = dot_nn(tril, jnp.broadcast_to(logd, (R, R)))
        Dm = jnp.where(lower, jnp.exp(jnp.where(lower, C - C.T, 0.0)), 0.0)
        N = dot_nt(k * beta, k) * Dm
        X = jnp.where(ri == rj, 1.0, 0.0) - jnp.where(levels[0], N, 0.0)
        for mask in levels[1:]:
            X = X - dot_nn(X, dot_nn(jnp.where(mask, N, 0.0), X))
        C64 = C[:, :E]
        ec = jnp.exp(C64)
        U = dot_nn(X, v * beta)
        W = dot_nn(X, k * beta * ec)
        last = C64[R - 1:R, :]
        kd = k * jnp.exp(last - C64)
        Pm = dot_nt(q, k) * Dm
        st[me, h, :, 0:E] = jnp.where(ei == ej, jnp.exp(last), 0.0) - dot_tn(kd, W)
        st[me, h, :, E:2 * E] = dot_tn(kd, U)
        keep.append((dot_nn(Pm, U), q * ec - dot_nn(Pm, W)))

    def st_copy(d, p):
        return pltpu.make_async_remote_copy(
            src_ref=st.at[p], dst_ref=st.at[p], send_sem=st_send.at[d], recv_sem=st_recv.at[p],
            device_id={"sp": lax.rem(me + d, S)}, device_id_type=MESH)

    relays(1, 1, Z)

    def st_start(d, _):
        st_copy(d, me).start()
        return 0
    lax.fori_loop(1, S - me, st_start, 0)
    finish(1)
    wproj = jnp.dot(normed[...], Ww[...], preferred_element_type=f32)

    def rope(u):
        return u * cosine + dot_nn(u, swap) * sine
    k_cur = rope(wproj[:, qc:qc + kc]).astype(bf16)
    v_cur = wproj[:, qc + kc:qc + 2 * kc].astype(bf16)
    edge_own[:, 0:kc] = k_cur
    edge_own[:, kc:2 * kc] = v_cur
    queries = [rope(wproj[:, h * E:(h + 1) * E]).astype(bf16) for h in range(QH)]

    def edge_copy():
        return pltpu.make_async_remote_copy(
            src_ref=edge_own, dst_ref=edge_in, send_sem=edge_send, recv_sem=edge_recv,
            device_id={"sp": lax.rem(me + 1, S)}, device_id_type=MESH)
    edge_copy().start()
    relays(2, 1, Z)
    edge_copy().wait_recv()
    k_prev = edge_in[:, 0:kc]
    v_prev = edge_in[:, kc:2 * kc]
    seen_prev = (rj > ri) & (me > 0)
    for h in range(QH):
        s_cur = jnp.where(lower, dot_nt(queries[h], k_cur, None) * E ** (-0.5), -jnp.inf)
        s_prev = jnp.where(seen_prev, dot_nt(queries[h], k_prev, None) * E ** (-0.5), -jnp.inf)
        sink = sink_ref[h]
        top = jnp.maximum(jnp.maximum(jnp.max(s_cur, axis=1, keepdims=True), jnp.max(s_prev, axis=1, keepdims=True)), sink)
        e_cur = jnp.exp(s_cur - top)
        e_prev = jnp.exp(s_prev - top)
        row_total = (jnp.sum(e_cur, axis=1, keepdims=True) + jnp.sum(e_prev, axis=1, keepdims=True)
                     + jnp.exp(sink - top))
        logt_ref[:, h:h + 1] = top + jnp.log(row_total)
        mixed_rows = (dot_nn((e_cur / row_total).astype(bf16), v_cur, None)
                      + dot_nn((e_prev / row_total).astype(bf16), v_prev, None))
        mix[:, dc + h * E:dc + (h + 1) * E] = mixed_rows.astype(bf16)

    def chain(p, carry):
        pltpu.make_async_remote_copy(
            src_ref=st.at[p], dst_ref=st.at[p], send_sem=st_send.at[0], recv_sem=st_recv.at[p],
            device_id={"sp": lax.rem(me + 1, S)}, device_id_type=MESH).wait_recv()
        for h in range(H):
            memory[h] = dot_nn(st[p, h, :, 0:E], memory[h]) + st[p, h, :, E:2 * E]
        return carry
    memory[...] = jnp.zeros(memory.shape, f32)
    lax.fori_loop(0, me, chain, 0)
    for h in range(H):
        o = keep[h][0] + dot_nn(keep[h][1], memory[h])
        o = o * lax.rsqrt(jnp.mean(o * o, axis=1, keepdims=True) + epsilon) * ngain_ref[...]
        gate = proj[:, 3 * dc + h * E:3 * dc + (h + 1) * E]
        mix[:, h * E:(h + 1) * E] = (o * silu(gate)).astype(bf16)

    finish(2)
    part[...] = dot_nt(mix[...], Wo[...], None).astype(bf16)
    r = R // T

    def out_copy(d, source):
        peer = lax.rem(j + d, T)
        return pltpu.make_async_remote_copy(
            src_ref=part.at[pl.ds(pl.multiple_of(peer * r, r), r), :], dst_ref=partin.at[source],
            send_sem=out_send.at[d], recv_sem=out_recv.at[source],
            device_id={"tp": peer}, device_id_type=MESH)
    for d in range(1, T):
        out_copy(d, j).start()
    partin[j] = part[pl.ds(pl.multiple_of(j * r, r), r), :]
    for d in range(1, T):
        out_copy(d, lax.rem(j + d, T)).wait_recv()
    acc = partin[0].astype(f32)
    for t in range(1, T):
        acc = acc + partin[t].astype(f32)
    mixed_ref[...] = acc.astype(bf16)

    for d in range(1, T):
        out_copy(d, j).wait_send()
        tok_copy(d).wait_send()
    edge_copy().wait_send()

    def st_done(d, _):
        st_copy(d, me).wait_send()
        return 0
    lax.fori_loop(1, S - me, st_done, 0)
    for g in range(3):
        drain(g)


def shards(S, T, tokens, gain, dq, dk, dv, dz, ww, wd, bias, scale, offs, ngain, do, wq, wk, wv, sink, wo):
    R, F = tokens.shape
    D = F * T
    dc = dq.shape[1]
    H = bias.shape[0]
    E = dc // H
    qc, kc = wq.shape[1], wk.shape[1]
    G = 2 if S % 2 == 0 else 1
    Z = S // G
    vmem = pl.BlockSpec(memory_space=pltpu.VMEM)
    smem = pl.BlockSpec(memory_space=pltpu.SMEM)
    hbm = pl.BlockSpec(memory_space=pl.ANY)
    dma = pltpu.SemaphoreType.DMA
    return pl.pallas_call(
        functools.partial(layer_kernel, S, T, G),
        out_shape=(jax.ShapeDtypeStruct((R // T, D), bf16), jax.ShapeDtypeStruct((R, sink.shape[0]), f32)),
        in_specs=[vmem, vmem, hbm, hbm, hbm, hbm, vmem, vmem, smem, smem, vmem, vmem, hbm, hbm, vmem, vmem, smem, hbm],
        out_specs=(vmem, vmem),
        scratch_shapes=[
            pltpu.VMEM((T, R, F), bf16),
            pltpu.VMEM((R, D), bf16),
            pltpu.VMEM((D, 4 * dc), bf16),
            pltpu.VMEM((D, qc + 2 * kc), bf16),
            pltpu.VMEM((D, dc + qc), bf16),
            pltpu.VMEM((S, H, E, 2 * E), f32),
            pltpu.VMEM((R, 2 * kc), bf16),
            pltpu.VMEM((R, 2 * kc), bf16),
            pltpu.VMEM((R, dc + qc), bf16),
            pltpu.VMEM((R, D), bf16),
            pltpu.VMEM((T, R // T, D), bf16),
            pltpu.VMEM((H, E, E), f32),
            dma((8,)), dma((T,)), dma((T,)), dma((3, 3, Z)), dma((3, S)), dma((S,)), dma((S,)),
            dma, dma, dma((T,)), dma((T,)),
        ],
        compiler_params=pltpu.CompilerParams(
            collective_id=0, has_side_effects=True, vmem_limit_bytes=60 * 1024 * 1024),
    )(tokens, gain.reshape(1, D), dq, dk, dv, dz, ww, wd, bias, scale, offs, ngain.reshape(1, E), do, wq, wk, wv, sink, wo)


def solution(mesh):
    both = P("sp", "tp")
    placed = (both, P(), both, both, both, both, P(), P(), P("tp"), P("tp"), both, P(), both, both, both, both,
              P("tp"), both)
    return jax.shard_map(
        functools.partial(shards, mesh.shape["sp"], mesh.shape["tp"]),
        mesh=mesh, in_specs=placed, out_specs=(P(("sp", "tp"), None), both), check_vma=False)
```

```python
import functools

import jax
import jax.numpy as jnp
from jax import lax
from jax.experimental import pallas as pl
from jax.experimental.pallas import tpu as pltpu
from jax.sharding import PartitionSpec as P

WINDOW = 128
epsilon = 1e-06
rope_base = 500000.0
highest = lax.Precision.HIGHEST
MESH = pl.DeviceIdType.MESH
f32 = jnp.float32
bf16 = jnp.bfloat16


def dot_nn(a, b, precision=highest):
    return lax.dot_general(a, b, (((1,), (0,)), ((), ())), precision=precision, preferred_element_type=f32)


def dot_nt(a, b, precision=highest):
    return lax.dot_general(a, b, (((1,), (1,)), ((), ())), precision=precision, preferred_element_type=f32)


def dot_tn(a, b, precision=highest):
    return lax.dot_general(a, b, (((0,), (0,)), ((), ())), precision=precision, preferred_element_type=f32)


def silu(u):
    return u / (1.0 + jnp.exp(-u))


def unit_rows(u):
    return u * lax.rsqrt(jnp.sum(u * u, axis=-1, keepdims=True) + epsilon)


def iota(shape, dim):
    return lax.broadcasted_iota(jnp.int32, shape, dim)


def layer_kernel(
    S, T, G,
    tok_ref, gain_ref, dq_ref, dk_ref, dv_ref, dz_ref, ww_ref, wd_ref, bias_ref, scale_ref, offs_ref,
    ngain_ref, do_ref, wq_ref, wk_ref, wv_ref, sink_ref, wo_ref,
    mixed_ref, logt_ref,
    tokbuf, feats, away, Wd, Ww, Wo, dpart, dpart_in, wpart, wpart_in, st, edge_own, edge_in, mix, part, partin,
    red, red_in, memory,
    local_sem, tok_send, tok_recv, w_send, w_recv, st_send, st_recv, edge_send, edge_recv, out_send, out_recv,
    pair_send, pair_recv,
):
    me = lax.axis_index("sp")
    j = lax.axis_index("tp")
    Z = S // G
    z = me // G
    x = me % G
    other = lax.rem(x + 1, G)
    R, F = tok_ref.shape
    rows = dq_ref.shape[0]
    K = Z * rows
    dc = dq_ref.shape[1]
    qc = wq_ref.shape[1]
    kc = wk_ref.shape[0]
    H = bias_ref.shape[0]
    E = dc // H
    QH = sink_ref.shape[0]
    mine = pl.ds(pl.multiple_of(z * rows, rows), rows)

    def local(i, src, dst):
        return pltpu.make_async_copy(src, dst, local_sem.at[i])

    locals_ = [
        local(0, dq_ref, Wd.at[mine, pl.ds(0, dc)]),
        local(1, dk_ref, Wd.at[mine, pl.ds(dc, dc)]),
        local(2, dv_ref, Wd.at[mine, pl.ds(2 * dc, dc)]),
        local(3, dz_ref, Wd.at[mine, pl.ds(3 * dc, dc)]),
        local(4, wq_ref, Ww.at[mine, pl.ds(0, qc)]),
        local(5, do_ref, Wo.at[mine, pl.ds(0, dc)]),
        local(6, wo_ref, Wo.at[mine, pl.ds(dc, qc)]),
        local(7, tok_ref, tokbuf.at[j]),
    ]
    for c in locals_:
        c.start()

    barrier = pltpu.get_barrier_semaphore()

    def greet_sp(d, _):
        pl.semaphore_signal(barrier, inc=1, device_id={"sp": lax.rem(me + d, S)}, device_id_type=MESH)
        return 0

    lax.fori_loop(1, S, greet_sp, 0)
    for d in range(1, T):
        pl.semaphore_signal(barrier, inc=1, device_id={"tp": lax.rem(j + d, T)}, device_id_type=MESH)
    narrow = jnp.concatenate([wk_ref[...], wv_ref[...]], axis=0).astype(f32)
    Ww[mine, pl.ds(qc, 2 * kc)] = narrow.T.astype(bf16)
    pl.semaphore_wait(barrier, S - 1 + T - 1)

    def tok_copy(d):
        return pltpu.make_async_remote_copy(
            src_ref=tok_ref, dst_ref=tokbuf.at[j], send_sem=tok_send.at[d], recv_sem=tok_recv.at[j],
            device_id={"tp": lax.rem(j + d, T)}, device_id_type=MESH)

    for d in range(1, T):
        tok_copy(d).start()

    def pair_copy(i, src, dst):
        return pltpu.make_async_remote_copy(
            src_ref=src, dst_ref=dst, send_sem=pair_send.at[i], recv_sem=pair_recv.at[i],
            device_id={"sp": me - x + other}, device_id_type=MESH)

    bufs = (Wd, Ww, Wo)

    def slab(g, zz):
        return bufs[g].at[pl.ds(pl.multiple_of(zz * rows, rows), rows), :]

    def wcopy(g, zz, way):
        return pltpu.make_async_remote_copy(
            src_ref=slab(g, zz), dst_ref=slab(g, zz), send_sem=w_send.at[g, way, zz], recv_sem=w_recv.at[g, zz],
            device_id={"sp": (me + G, me - G)[way]}, device_id_type=MESH)

    def forward(g, zz, up, down):
        if up:
            @pl.when(z + 1 < Z)
            def _():
                wcopy(g, zz, 0).start()
        if down:
            @pl.when(z > 0)
            def _():
                wcopy(g, zz, 1).start()

    def relay(g, t):
        @pl.when(z - t >= 0)
        def _():
            wcopy(g, z - t, 0).wait_recv()
            forward(g, z - t, True, False)

        @pl.when(z + t < Z)
        def _():
            wcopy(g, z + t, 0).wait_recv()
            forward(g, z + t, False, True)

    def relays(g, low, high):
        def one(t, _):
            relay(g, t)
            return 0
        lax.fori_loop(low, high, one, 0)

    def drain(g):
        def one(zz, _):
            @pl.when((zz <= z) & (z + 1 < Z))
            def _():
                wcopy(g, zz, 0).wait_send()

            @pl.when((zz >= z) & (z > 0))
            def _():
                wcopy(g, zz, 1).wait_send()
            return 0
        lax.fori_loop(0, Z, one, 0)

    for i in range(4):
        locals_[i].wait()
    forward(0, z, True, True)

    half = E // 2
    lane = iota((R, E), 1)
    pair = jnp.where(lane < half, lane, lane - half).astype(f32)
    frequency = jnp.exp(pair * (-(2.0 / E)) * jnp.log(jnp.full((R, E), rope_base, f32)))
    angle = (me * R + iota((R, E), 0)).astype(f32) * frequency
    cosine = jnp.cos(angle)
    sine = jnp.sin(angle)
    ei = iota((E, E), 0)
    ej = iota((E, E), 1)
    swap = jnp.where(ei == ej + half, -1.0, 0.0) + jnp.where(ej == ei + half, 1.0, 0.0)

    locals_[7].wait()
    for d in range(1, T):
        src = lax.rem(j + d, T)
        pltpu.make_async_remote_copy(
            src_ref=tok_ref, dst_ref=tokbuf.at[src], send_sem=tok_send.at[d], recv_sem=tok_recv.at[src],
            device_id={"tp": lax.rem(j + d, T)}, device_id_type=MESH).wait_recv()
    total = jnp.zeros((R, 1), f32)
    for t in range(T):
        u = tokbuf[t].astype(f32)
        total = total + jnp.sum(u * u, axis=1, keepdims=True)
    inverse = lax.rsqrt(total / (T * F) + epsilon)
    pre_w = jnp.zeros((R, ww_ref.shape[0]), f32)
    pre_d = jnp.zeros((R, wd_ref.shape[0]), f32)
    wide = rows if G > 1 else F
    for g in range(G):
        c = lax.rem(x + g + 1, G) if G > 1 else 0
        for t in range(T * F // (wide * G)):
            at = t * wide * G + c * wide
            inner = pl.ds(pl.multiple_of(at % F, 128) if G > 1 else at % F, wide)
            cols = pl.ds(pl.multiple_of(at, 128) if G > 1 else at, wide)
            tok = tokbuf[t * wide * G // F, :, inner].astype(f32)
            piece = (tok * inverse * gain_ref[:, cols]).astype(bf16)
            pre_w = pre_w + dot_nt(piece, ww_ref[:, cols], None)
            pre_d = pre_d + dot_nt(piece, wd_ref[:, cols], None)
            if g + 1 == G:
                feats[x, :, t * wide:(t + 1) * wide] = piece
            else:
                away[:, t * wide:(t + 1) * wide] = piece
        if g + 1 < G:
            pair_copy(0, away, feats.at[x]).start()
    all_heads = pre_w.shape[1]
    head_lane = iota((R, all_heads), 1)

    relays(0, 1, Z)
    locals_[4].wait()
    forward(1, z, True, True)

    def project(i, weight, mine_out, landing):
        if G == 1:
            return jnp.dot(feats[0], weight[...], preferred_element_type=f32)
        mine_out[...] = jnp.dot(feats[other], weight[...], preferred_element_type=f32)
        pair_copy(i, mine_out, landing).start()
        half_sum = jnp.dot(feats[x], weight[...], preferred_element_type=f32)
        pair_copy(i, mine_out, landing).wait_recv()
        return half_sum + landing[...]

    if G > 1:
        pair_copy(0, away, feats.at[other]).wait_recv()
    proj = project(1, Wd, dpart, dpart_in)

    ri = iota((R, R), 0)
    rj = iota((R, R), 1)
    lower = ri >= rj
    strict = ri > rj
    tril = jnp.where(lower, 1.0, 0.0)
    levels = []
    size = 1
    while size < R:
        levels.append(strict & (ri // (2 * size) == rj // (2 * size)) & (ri // size != rj // size))
        size *= 2
    keep = []
    for h in range(H):
        if h > 0 and Z > 2:
            relay(1, h)

        def head(n):
            return proj[:, n * dc + h * E:n * dc + (h + 1) * E]
        q = unit_rows(silu(head(0))) * E ** (-0.5)
        k = unit_rows(silu(head(1)))
        v = silu(head(2))
        chosen = head_lane == j * H + h
        write = jnp.sum(jnp.where(chosen, pre_w, 0.0), axis=1, keepdims=True) + bias_ref[h]
        decay = jnp.sum(jnp.where(chosen, pre_d, 0.0), axis=1, keepdims=True)
        beta = 1.0 / (1.0 + jnp.exp(-write))
        soft = jnp.maximum(decay, 0.0) + jnp.log1p(jnp.exp(-jnp.abs(decay)))
        logd = jnp.broadcast_to(offs_ref[h:h + 1, :], (R, R)).T - scale_ref[h] * soft
        C = dot_nn(tril, logd)
        Dm = jnp.where(lower, jnp.exp(jnp.where(lower, C - C.T, 0.0)), 0.0)
        N = dot_nt(k * beta, k) * Dm
        X = jnp.where(ri == rj, 1.0, 0.0) - jnp.where(levels[0], N, 0.0)
        for mask in levels[1:]:
            X = X - dot_nn(X, dot_nn(jnp.where(mask, N, 0.0), X))
        C64 = C[:, :E]
        ec = jnp.exp(C64)
        U = dot_nn(X, v * beta)
        W = dot_nn(X, k * beta * ec)
        last = C64[R - 1:R, :]
        kd = k * jnp.exp(last - C64)
        Pm = dot_nt(q, k) * Dm
        st[me, h, :, 0:E] = jnp.where(ei == ej, jnp.exp(last), 0.0) - dot_tn(kd, W)
        st[me, h, :, E:2 * E] = dot_tn(kd, U)
        keep.append((dot_nn(Pm, U), q * ec - dot_nn(Pm, W)))

    def st_copy(d, p):
        return pltpu.make_async_remote_copy(
            src_ref=st.at[p], dst_ref=st.at[p], send_sem=st_send.at[d], recv_sem=st_recv.at[p],
            device_id={"sp": lax.rem(me + d, S)}, device_id_type=MESH)

    def st_start(d, _):
        st_copy(d, me).start()
        return 0
    relays(1, H if Z > 2 else 1, Z)
    lax.fori_loop(1, S - me, st_start, 0)
    for i in (5, 6):
        locals_[i].wait()
    forward(2, z, True, True)
    wproj = project(2, Ww, wpart, wpart_in)

    def rope(u):
        return u * cosine + dot_nn(u, swap) * sine
    k_cur = rope(wproj[:, qc:qc + kc]).astype(bf16)
    v_cur = wproj[:, qc + kc:qc + 2 * kc].astype(bf16)
    edge_own[:, 0:kc] = k_cur
    edge_own[:, kc:2 * kc] = v_cur
    queries = [rope(wproj[:, h * E:(h + 1) * E]).astype(bf16) for h in range(QH)]

    def edge_copy():
        return pltpu.make_async_remote_copy(
            src_ref=edge_own, dst_ref=edge_in, send_sem=edge_send, recv_sem=edge_recv,
            device_id={"sp": lax.rem(me + 1, S)}, device_id_type=MESH)
    edge_copy().start()
    if Z > 1:
        relay(2, 1)
    edge_copy().wait_recv()
    k_prev = edge_in[:, 0:kc]
    v_prev = edge_in[:, kc:2 * kc]
    seen_prev = (rj > ri) & (me > 0)
    for h in range(QH):
        s_cur = jnp.where(lower, dot_nt(queries[h], k_cur, None) * E ** (-0.5), -jnp.inf)
        s_prev = jnp.where(seen_prev, dot_nt(queries[h], k_prev, None) * E ** (-0.5), -jnp.inf)
        sink = sink_ref[h]
        top = jnp.maximum(jnp.maximum(jnp.max(s_cur, axis=1, keepdims=True), jnp.max(s_prev, axis=1, keepdims=True)), sink)
        e_cur = jnp.exp(s_cur - top)
        e_prev = jnp.exp(s_prev - top)
        row_total = (jnp.sum(e_cur, axis=1, keepdims=True) + jnp.sum(e_prev, axis=1, keepdims=True)
                     + jnp.exp(sink - top))
        logt_ref[:, h:h + 1] = top + jnp.log(row_total)
        if h == 1 and Z > 2:
            relay(2, 2)
        mixed_rows = (dot_nn((e_cur / row_total).astype(bf16), v_cur, None)
                      + dot_nn((e_prev / row_total).astype(bf16), v_prev, None))
        mix[x, :, dc + h * E:dc + (h + 1) * E] = mixed_rows.astype(bf16)

    relays(2, min(3 if QH > 1 else 2, Z), Z)
    def chain(p, carry):
        pltpu.make_async_remote_copy(
            src_ref=st.at[p], dst_ref=st.at[p], send_sem=st_send.at[0], recv_sem=st_recv.at[p],
            device_id={"sp": lax.rem(me + 1, S)}, device_id_type=MESH).wait_recv()
        for h in range(H):
            memory[h] = dot_nn(st[p, h, :, 0:E], memory[h]) + st[p, h, :, E:2 * E]
        return carry
    memory[...] = jnp.zeros(memory.shape, f32)
    lax.fori_loop(0, me, chain, 0)
    for h in range(H):
        o = keep[h][0] + dot_nn(keep[h][1], memory[h])
        o = o * lax.rsqrt(jnp.mean(o * o, axis=1, keepdims=True) + epsilon) * ngain_ref[...]
        gate = proj[:, 3 * dc + h * E:3 * dc + (h + 1) * E]
        mix[x, :, h * E:(h + 1) * E] = (o * silu(gate)).astype(bf16)

    if G > 1:
        pair_copy(3, mix.at[x], mix.at[x]).start()
        part[x] = dot_nt(mix[x], Wo[...], None).astype(bf16)
        pair_copy(3, mix.at[x], mix.at[other]).wait_recv()
        part[other] = dot_nt(mix[other], Wo[...], None).astype(bf16)
    else:
        part[0] = dot_nt(mix[0], Wo[...], None).astype(bf16)
    r = R // T

    def out_copy(d, source):
        peer = lax.rem(j + d, T)
        return pltpu.make_async_remote_copy(
            src_ref=part.at[:, pl.ds(pl.multiple_of(peer * r, r), r), :], dst_ref=partin.at[source],
            send_sem=out_send.at[d], recv_sem=out_recv.at[source],
            device_id={"tp": peer}, device_id_type=MESH)
    for d in range(1, T):
        out_copy(d, j).start()
    partin[j] = part[:, pl.ds(pl.multiple_of(j * r, r), r), :]
    for d in range(1, T):
        out_copy(d, lax.rem(j + d, T)).wait_recv()

    def reduced(slot):
        acc = partin[0, slot].astype(f32)
        for t in range(1, T):
            acc = acc + partin[t, slot].astype(f32)
        return acc.astype(bf16)
    if G > 1:
        red[...] = reduced(other)
        pair_copy(4, red, red_in).start()
        done = reduced(x)
        for zz in range(Z):
            at = pl.multiple_of(zz * G * rows + x * rows, 128)
            mixed_ref[:, pl.ds(at, rows)] = done[:, zz * rows:(zz + 1) * rows]
        pair_copy(4, red, red_in).wait_recv()
        for zz in range(Z):
            at = pl.multiple_of(zz * G * rows + other * rows, 128)
            mixed_ref[:, pl.ds(at, rows)] = red_in[:, zz * rows:(zz + 1) * rows]
        pair_copy(0, away, feats.at[x]).wait_send()
        pair_copy(1, dpart, dpart_in).wait_send()
        pair_copy(2, wpart, wpart_in).wait_send()
        pair_copy(3, mix.at[x], mix.at[x]).wait_send()
        pair_copy(4, red, red_in).wait_send()
    else:
        mixed_ref[...] = reduced(0)

    for d in range(1, T):
        out_copy(d, j).wait_send()
        tok_copy(d).wait_send()
    edge_copy().wait_send()

    def st_done(d, _):
        st_copy(d, me).wait_send()
        return 0
    lax.fori_loop(1, S - me, st_done, 0)
    for g in range(3):
        drain(g)


def shards(S, T, tokens, gain, dq, dk, dv, dz, ww, wd, bias, scale, offs, ngain, do, wq, wk, wv, sink, wo):
    R, F = tokens.shape
    D = F * T
    rows = dq.shape[0]
    dc = dq.shape[1]
    H = bias.shape[0]
    E = dc // H
    qc, kc = wq.shape[1], wk.shape[1]
    G = 2 if S % 2 == 0 and rows % 128 == 0 and F % (2 * rows) == 0 else 1
    Z = S // G
    K = D // G
    vmem = pl.BlockSpec(memory_space=pltpu.VMEM)
    smem = pl.BlockSpec(memory_space=pltpu.SMEM)
    hbm = pl.BlockSpec(memory_space=pl.ANY)
    dma = pltpu.SemaphoreType.DMA
    V = pltpu.VMEM
    return pl.pallas_call(
        functools.partial(layer_kernel, S, T, G),
        out_shape=(jax.ShapeDtypeStruct((R // T, D), bf16), jax.ShapeDtypeStruct((R, sink.shape[0]), f32)),
        in_specs=[vmem, vmem, hbm, hbm, hbm, hbm, vmem, vmem, smem, smem, vmem, vmem, hbm, hbm, vmem, vmem, smem, hbm],
        out_specs=(vmem, vmem),
        scratch_shapes=[
            V((T, R, F), bf16),
            V((G, R, K), bf16),
            V((R, K), bf16),
            V((K, 4 * dc), bf16),
            V((K, qc + 2 * kc), bf16),
            V((K, dc + qc), bf16),
            V((R, 4 * dc), f32),
            V((R, 4 * dc), f32),
            V((R, qc + 2 * kc), f32),
            V((R, qc + 2 * kc), f32),
            V((S, H, E, 2 * E), f32),
            V((R, 2 * kc), bf16),
            V((R, 2 * kc), bf16),
            V((G, R, dc + qc), bf16),
            V((G, R, K), bf16),
            V((T, G, R // T, K), bf16),
            V((R // T, K), bf16),
            V((R // T, K), bf16),
            V((H, E, E), f32),
            dma((8,)), dma((T,)), dma((T,)), dma((3, 2, Z)), dma((3, Z)), dma((S,)), dma((S,)),
            dma, dma, dma((T,)), dma((T,)), dma((5,)), dma((5,)),
        ],
        compiler_params=pltpu.CompilerParams(
            collective_id=0, has_side_effects=True, vmem_limit_bytes=60 * 1024 * 1024),
    )(tokens, gain.reshape(1, D), dq, dk, dv, dz, ww.T, wd.T, bias, scale, offs.T, ngain.reshape(1, E), do, wq, wk.T,
      wv.T, sink, wo)


def solution(mesh):
    both = P("sp", "tp")
    placed = (both, P(), both, both, both, both, P(), P(), P("tp"), P("tp"), both, P(), both, both, both, both,
              P("tp"), both)
    return jax.shard_map(
        functools.partial(shards, mesh.shape["sp"], mesh.shape["tp"]),
        mesh=mesh, in_specs=placed, out_specs=(P(("sp", "tp"), None), both), check_vma=False)
```
